32 devices in a mesh: kv: 8 (over z, x), tp: 4 (over y, core).
Axes of the slice: x: 2, y: 2, z: 4, core: 2. Of those that a mesh axis runs over, the one named last changes fastest.
Arguments:
- tokens: bfloat16 [8192, 2048], P('kv'), may hold values from -72 to 72
- query_weight: bfloat16 [2048, 2048], P(None, 'tp'), may hold values from -0.125 to 0.125
- key_projection_matrix: bfloat16 [2048, 1024], P(None, 'tp'), may hold values from -0.125 to 0.125
- value_projection_matrix: bfloat16 [2048, 1024], P(None, 'tp'), may hold values from -0.125 to 0.125
- out_weight: bfloat16 [2048, 2048], P('tp'), may hold values from -1.5 to 1.5
- chosen: int32 [64, 12], P('kv'), may hold values from -1 to 255, as said below
Outputs:
- layer_out: bfloat16 [8192, 2048], P(('kv', 'tp'))
The draws below stay inside these ranges and needn't reach their ends.
Inputs may be any that keep to these rules, and one draw needn't show every extreme that they name: `chosen`: positions are grouped in consecutive groups of 1024. The blocks named in one row lie in distinct groups, all earlier than the group of the row's query block; a query block in group g has exactly min(12, g) entries that are not -1, first in its row, and the rest are -1. So the query blocks of one group name at most 8 blocks of any one other group, and in every draw some group's query blocks all name blocks of one same earlier group.
All inputs are finite; a program needn't handle non-finite values.
Results may differ from the reference program's by a relative error of at most 0.014.
The reference program's roundings to bfloat16 on the way count: a program that leaves them out, or rounds other values in their place, can miss the bound.
Values may be sent and summed in bfloat16 or wider, within the bound.
A program may use at most 64 MiB of HBM per device.

```python
import jax
import jax.numpy as jnp
from jax import lax

MODEL_WIDTH = 2048
QUERY_HEADS = 16
KEY_VALUE_HEADS = 8
HEAD_SIZE = 128
TOK_DEV = 1024
QUERY_BLOCK_SPAN = 128
KEY_BLOCK_SPAN = 32
NFAR = 12
SEQUENCE_TOKENS = 8192
N_TP = 4


def draw_tokens(key, part):
    split_keys = jax.random.split(jax.random.fold_in(key, 11), 3)
    base_rows = jnp.clip(jax.random.normal(split_keys[0], (SEQUENCE_TOKENS, MODEL_WIDTH), jnp.float32), -6.0, 6.0)
    return base_rows.astype(jnp.bfloat16)


def draw_chosen(key, part):
    group_count = SEQUENCE_TOKENS // TOK_DEV
    per_group = TOK_DEV // QUERY_BLOCK_SPAN
    blocks_per_group = TOK_DEV // KEY_BLOCK_SPAN
    query_count = SEQUENCE_TOKENS // QUERY_BLOCK_SPAN
    split_keys = jax.random.split(jax.random.fold_in(key, 7), 4)
    owner_ids = jnp.arange(group_count, dtype=jnp.int32)
    home_group = jnp.arange(query_count, dtype=jnp.int32) // per_group
    first_local = jnp.arange(query_count, dtype=jnp.int32) % per_group == 0
    popular = jax.random.randint(split_keys[0], (group_count,), 0, 3) * (1 << 19)
    jitter = jax.random.randint(split_keys[1], (query_count, group_count), 0, 1 << 20)
    favoured = jax.random.randint(split_keys[2], (group_count,), 0, 1 << 20) % jnp.maximum(owner_ids, 1)
    source = home_group[:, None]
    target = owner_ids[None, :]
    forced = (target == favoured[home_group][:, None]) | first_local[:, None] & ((target == source - 1) | (target == source - group_count // 2))
    ranking = (jitter + popular[None, :]) * group_count + target
    ranking = jnp.where(forced, ranking + (1 << 29), ranking)
    ranking = jnp.where(target < source, ranking, -1)
    take_count = min(NFAR, group_count)
    best_scores, picked_owner = lax.top_k(ranking, take_count)
    inner_ids = jax.random.randint(split_keys[3], (query_count, take_count), 0, blocks_per_group)
    listed = jnp.where(best_scores >= 0, picked_owner.astype(jnp.int32) * blocks_per_group + inner_ids, -1)
    if take_count < NFAR:
        padding = jnp.full((query_count, NFAR - take_count), -1, jnp.int32)
        listed = jnp.concatenate([listed, padding], axis=1)
    return listed.astype(jnp.int32)


def steps_of(own_key, extent, cuts, smallest, high):
    def one(axis_at, shards_of):
        heights = jax.random.uniform(jax.random.fold_in(jax.random.fold_in(own_key, 6), axis_at), (shards_of,), jnp.float32, smallest / len(cuts), high / len(cuts))
        return jnp.repeat(jnp.exp(heights), extent[axis_at] // shards_of).reshape((-1,) + (1,) * (len(extent) - axis_at - 1))

    loudness = one(*cuts[0])
    for cut in cuts[1:]:
        loudness = loudness * one(*cut)
    return loudness


def bell_draw(rng, dims, scale, reach, pieces=(), kind=jnp.bfloat16):
    result = scale * jax.random.normal(rng, dims, jnp.float32)
    if pieces:
        result = result * steps_of(rng, dims, pieces, -0.22, 0.18)
    return jnp.clip(result, -reach, reach).astype(kind)


def setup_inputs(seed: int = 0) -> dict:
    arg_keys = jax.random.split(jax.random.key(seed), 7)
    return {
        "tokens": draw_tokens(jax.random.fold_in(arg_keys[6], 71), 0),
        "query_weight": bell_draw(arg_keys[1], (MODEL_WIDTH, QUERY_HEADS * HEAD_SIZE), MODEL_WIDTH ** -0.5, 0.125, ((1, 4),)),
        "key_projection_matrix": bell_draw(arg_keys[2], (MODEL_WIDTH, KEY_VALUE_HEADS * HEAD_SIZE), MODEL_WIDTH ** -0.5, 0.125, ((1, 4),)),
        "value_projection_matrix": bell_draw(arg_keys[3], (MODEL_WIDTH, KEY_VALUE_HEADS * HEAD_SIZE), MODEL_WIDTH ** -0.5, 0.125, ((1, 4),)),
        "out_weight": bell_draw(arg_keys[4], (QUERY_HEADS * HEAD_SIZE, MODEL_WIDTH), (HEAD_SIZE // 8) ** -0.5, 1.5, ((0, 4),)),
        "chosen": draw_chosen(jax.random.fold_in(arg_keys[6], 71), 0),
    }


def reference(tokens, query_weight, key_projection_matrix, value_projection_matrix, out_weight, chosen):
    queries = jnp.dot(tokens, query_weight, preferred_element_type=jnp.float32).astype(jnp.bfloat16)
    key_vectors = jnp.dot(tokens, key_projection_matrix, preferred_element_type=jnp.float32).astype(jnp.bfloat16)
    value_vectors = jnp.dot(tokens, value_projection_matrix, preferred_element_type=jnp.float32).astype(jnp.bfloat16)
    grouped_head_index = QUERY_HEADS // KEY_VALUE_HEADS
    diag_blocks = QUERY_BLOCK_SPAN // KEY_BLOCK_SPAN
    blocked_keys = key_vectors.reshape(SEQUENCE_TOKENS // KEY_BLOCK_SPAN, KEY_BLOCK_SPAN, KEY_VALUE_HEADS * HEAD_SIZE)
    blocked_values = value_vectors.reshape(SEQUENCE_TOKENS // KEY_BLOCK_SPAN, KEY_BLOCK_SPAN, KEY_VALUE_HEADS * HEAD_SIZE)
    offsets = jnp.arange(KEY_BLOCK_SPAN, dtype=jnp.int32)
    row_ids = jnp.arange(QUERY_BLOCK_SPAN, dtype=jnp.int32)

    def one_block(block_index):
        first_row = block_index * QUERY_BLOCK_SPAN
        queries_in_block = lax.dynamic_slice_in_dim(queries, first_row, QUERY_BLOCK_SPAN, 0)
        queries_in_block = queries_in_block.reshape(QUERY_BLOCK_SPAN, KEY_VALUE_HEADS, grouped_head_index, HEAD_SIZE).astype(jnp.float32)
        picked = lax.dynamic_slice_in_dim(chosen, block_index, 1, 0)[0]
        block_ids = jnp.concatenate([block_index * diag_blocks + jnp.arange(diag_blocks, dtype=jnp.int32), picked])
        is_valid = block_ids >= 0
        guarded_block_index = jnp.maximum(block_ids, 0)
        key_pos = (guarded_block_index[:, None] * KEY_BLOCK_SPAN + offsets[None, :]).reshape(-1)
        key_ok = jnp.broadcast_to(is_valid[:, None], (block_ids.shape[0], KEY_BLOCK_SPAN)).reshape(-1)
        query_pos = first_row + row_ids
        allowed = key_ok[None, :] & (key_pos[None, :] <= query_pos[:, None])
        nearby_keys = blocked_keys[guarded_block_index].reshape(-1, KEY_VALUE_HEADS, HEAD_SIZE).astype(jnp.float32)
        nearby_values = blocked_values[guarded_block_index].reshape(-1, KEY_VALUE_HEADS, HEAD_SIZE).astype(jnp.float32)
        scores = jnp.einsum("qgrd,kgd->grqk", queries_in_block, nearby_keys, precision=lax.Precision.HIGHEST) * (HEAD_SIZE ** -0.5)
        scores = jnp.where(allowed[None, None], scores, -jnp.inf)
        row_max = jnp.max(scores, axis=-1, keepdims=True)
        exp_scores = jnp.exp(scores - row_max)
        row_sum = jnp.sum(exp_scores, axis=-1, keepdims=True)
        weights = (exp_scores / row_sum).astype(jnp.bfloat16)
        mixed = jnp.einsum("grqk,kgd->qgrd", weights.astype(jnp.float32), nearby_values, precision=lax.Precision.HIGHEST)
        return mixed.astype(jnp.bfloat16).reshape(QUERY_BLOCK_SPAN, QUERY_HEADS * HEAD_SIZE)

    all_blocks = lax.map(one_block, jnp.arange(SEQUENCE_TOKENS // QUERY_BLOCK_SPAN, dtype=jnp.int32))
    attended = all_blocks.reshape(SEQUENCE_TOKENS, QUERY_HEADS * HEAD_SIZE)
    slice_width = QUERY_HEADS * HEAD_SIZE // N_TP
    summed = jnp.zeros((SEQUENCE_TOKENS, MODEL_WIDTH), jnp.float32)
    for part_index in range(N_TP):
        lower = part_index * slice_width
        partial_value = jnp.dot(attended[:, lower:lower + slice_width], out_weight[lower:lower + slice_width],
                          preferred_element_type=jnp.float32)
        rounded = lax.optimization_barrier(partial_value.astype(jnp.bfloat16))
        summed = summed + rounded.astype(jnp.float32)
    return summed.astype(jnp.bfloat16)
```

```python
import functools

import jax
import jax.numpy as jnp
from jax import lax
from jax.experimental import pallas as pl
from jax.experimental.pallas import tpu as pltpu
from jax.sharding import PartitionSpec as P

HEAD = 128
QB = 128
KB = 32
PIECES = 4
ROWS = 256
BF = jnp.bfloat16
F32 = jnp.float32
MESH = pl.DeviceIdType.MESH


def block_pairs(blocks):
    half = blocks // 2
    firsts = list(range(0, half, 2)) + list(range(1, half, 2))
    return [(i, i + half) for i in firsts]


def kernel(
    nkv, ntp, nfar,
    tok_hbm, wq_hbm, wk_hbm, wv_hbm, wo_hbm, list_v, list_s,
    out_ref,
    tok, wq, wk, wv, wo, q, kv, att, attr, kall, tmine, trecv, tsm, stage, *rest,
):
    chunks = block_pairs(att.shape[0])
    nch = len(chunks)
    recv = rest[:nch]
    (loc_sem, tok_sem, ts_sem, tr_sem, tl_sem, zs_sem, zr_sem,
     as_sem, ar_sem, cs_sem, cr_sem, ys_sem, yr_sem, rs_sem, rr_sem) = rest[nch:]
    me = lax.axis_index("kv")
    tp = lax.axis_index("tp")
    blocks = att.shape[0]
    bpm = attr.shape[1]
    kvw = wk.shape[1]
    kv_heads = kvw // HEAD
    qw = wq.shape[1]
    group = qw // kvw
    bpg = kv.shape[0]
    steps = tok.shape[0] // ROWS
    per_step = ROWS // KB
    kd = wo.shape[1]
    ny = ntp // 2
    mate = tp + 1 - 2 * lax.rem(tp, 2)

    load_wk = pltpu.make_async_copy(wk_hbm, wk, loc_sem.at[0])
    load_wv = pltpu.make_async_copy(wv_hbm, wv, loc_sem.at[1])
    load_wq = pltpu.make_async_copy(wq_hbm, wq, loc_sem.at[2])
    load_wo = pltpu.make_async_copy(wo_hbm, wo.at[tp], loc_sem.at[3])

    def load_tok(s):
        rows = pl.ds(s * ROWS, ROWS)
        return pltpu.make_async_copy(tok_hbm.at[rows, :], tok.at[rows, :], tok_sem.at[s])

    load_wk.start()
    load_tok(0).start()
    load_wv.start()
    for s in range(1, steps):
        load_tok(s).start()

    barrier = pltpu.get_barrier_semaphore()

    def greet(i, c):
        other = lax.rem(me + i, nkv)
        pl.semaphore_signal(barrier, inc=1, device_id={"kv": other, "tp": tp}, device_id_type=MESH)
        return c

    lax.fori_loop(1, nkv, greet, 0)
    for i in range(1, ntp):
        pl.semaphore_signal(
            barrier, inc=1, device_id={"kv": me, "tp": lax.rem(tp + i, ntp)}, device_id_type=MESH
        )

    named = list_v[...]
    lane = lax.broadcasted_iota(jnp.int32, tmine.shape, 1)
    table = jnp.zeros(tmine.shape, jnp.int32)
    for p in range(nkv):
        local = named - p * bpg
        mine = (local >= 0) & (local < bpg)
        column = jnp.sum(jnp.where(mine, local, 0), axis=1, keepdims=True)
        table = jnp.where(lane == p, column, table)
    tmine[...] = table
    load_wq.start()
    load_wo.start()
    pl.semaphore_wait(barrier, nkv + ntp - 2)

    def table_copy(p):
        return pltpu.make_async_remote_copy(
            src_ref=tmine, dst_ref=trecv.at[me], send_sem=ts_sem.at[p], recv_sem=tr_sem.at[me],
            device_id={"kv": p, "tp": tp}, device_id_type=MESH,
        )

    def table_in(d):
        return pltpu.make_async_remote_copy(
            src_ref=tmine, dst_ref=trecv.at[d], send_sem=ts_sem.at[d], recv_sem=tr_sem.at[d],
            device_id={"kv": d, "tp": tp}, device_id_type=MESH,
        )

    def table_local(d):
        return pltpu.make_async_copy(trecv.at[d], tsm.at[d], tl_sem.at[d])

    def each(lower, upper, action):
        def body(i, c):
            action(i)
            return c

        lax.fori_loop(lower, upper, body, 0)

    each(0, me, lambda p: table_copy(p).start())

    piece = kd // PIECES
    mate_copy = pltpu.make_async_remote_copy(
        src_ref=wo_hbm, dst_ref=wo.at[tp], send_sem=cs_sem, recv_sem=cr_sem,
        device_id={"kv": me, "tp": mate}, device_id_type=MESH,
    )
    mate_in = pltpu.make_async_remote_copy(
        src_ref=wo_hbm, dst_ref=wo.at[mate], send_sem=cs_sem, recv_sem=cr_sem,
        device_id={"kv": me, "tp": mate}, device_id_type=MESH,
    )

    def far_copy(dy, i):
        rows = pl.ds(i * piece, piece)
        return pltpu.make_async_remote_copy(
            src_ref=wo_hbm.at[rows, :], dst_ref=wo.at[tp, rows, :],
            send_sem=ys_sem.at[dy, i], recv_sem=yr_sem.at[dy, i],
            device_id={"kv": me, "tp": lax.rem(tp + 2 * dy, ntp)}, device_id_type=MESH,
        )

    def relay(dy, i, owner):
        rows = pl.ds(i * piece, piece)
        return pltpu.make_async_remote_copy(
            src_ref=wo.at[owner, rows, :], dst_ref=wo.at[owner, rows, :],
            send_sem=rs_sem.at[dy, i], recv_sem=rr_sem.at[dy, i],
            device_id={"kv": me, "tp": mate}, device_id_type=MESH,
        )

    def sender_of(who, dy):
        return lax.rem(who - 2 * dy + ntp, ntp)

    def start_piece(i):
        for dy in range(1, ny):
            far_copy(dy, i).start()

    def relay_piece(i):
        for dy in range(1, ny):
            far_copy(dy, i).wait_recv()
            relay(dy, i, sender_of(tp, dy)).start()

    mate_copy.start()
    start_piece(0)
    start_piece(1)

    load_wk.wait()
    load_wv.wait()

    def project_kv(s):
        load_tok(s).wait()
        x = tok[pl.ds(s * ROWS, ROWS), :]
        k = jnp.dot(x, wk[...], preferred_element_type=F32).astype(BF)
        v = jnp.dot(x, wv[...], preferred_element_type=F32).astype(BF)
        where = pl.ds(s * per_step, per_step)
        kv[where, :, :kvw] = k.reshape(per_step, KB, kvw)
        kv[where, :, kvw:] = v.reshape(per_step, KB, kvw)

    each(0, steps, project_kv)

    def table_got(d):
        table_in(d).wait_recv()
        table_local(d).start()

    each(me + 1, nkv, table_got)
    each(me + 1, nkv, lambda d: table_local(d).wait())

    def send_copy(c, d):
        return pltpu.make_async_remote_copy(
            src_ref=stage.at[c, d], dst_ref=recv[c].at[me],
            send_sem=zs_sem.at[c, d], recv_sem=zr_sem.at[c, me],
            device_id={"kv": d, "tp": tp}, device_id_type=MESH,
        )

    def arrive(c, p):
        return pltpu.make_async_remote_copy(
            src_ref=stage.at[c, p], dst_ref=recv[c].at[p],
            send_sem=zs_sem.at[c, p], recv_sem=zr_sem.at[c, p],
            device_id={"kv": p, "tp": tp}, device_id_type=MESH,
        )

    later = nkv - 1 - me
    for c, pair in enumerate(chunks):

        def stage_one(i, c=c, pair=pair):
            d = nkv - 1 - i
            for slot, b in enumerate(pair):
                stage[c, d, slot] = kv[tsm[d, b, me]]

        each(0, later, stage_one)
        each(0, later, lambda i, c=c: send_copy(c, nkv - 1 - i).start())

    load_wq.wait()

    def project_q(s):
        rows = pl.ds(s * ROWS, ROWS)
        q[rows, :] = jnp.dot(tok[rows, :], wq[...], preferred_element_type=F32).astype(BF)

    each(0, steps, project_q)

    keys = kall.shape[1]
    used = QB + nfar * KB
    row = lax.broadcasted_iota(jnp.int32, (QB, keys), 0)
    col = lax.broadcasted_iota(jnp.int32, (QB, keys), 1)
    count = jnp.minimum(nfar, me)
    allowed = (col <= row) | ((col >= QB) & (col < QB + KB * count))
    allowed = jnp.concatenate([allowed.astype(jnp.int32)] * group, axis=0) > 0
    if keys > used:
        for slot in range(len(chunks[0])):
            kall[slot, used:, :] = jnp.zeros((keys - used, 2 * kvw), BF)
    scale = HEAD ** (-0.5)

    def attend(b, slot):
        parts = []
        for g in range(kv_heads):
            first = g * group
            qs = jnp.concatenate(
                [q[b * QB:(b + 1) * QB, (first + r) * HEAD:(first + r + 1) * HEAD] for r in range(group)],
                axis=0,
            )
            ks = kall[slot, :, g * HEAD:(g + 1) * HEAD]
            vs = kall[slot, :, kvw + g * HEAD:kvw + (g + 1) * HEAD]
            s = lax.dot_general(qs, ks, (((1,), (1,)), ((), ())), preferred_element_type=F32) * scale
            s = jnp.where(allowed, s, -jnp.inf)
            e = jnp.exp(s - jnp.max(s, axis=-1, keepdims=True))
            w = (e * (1.0 / jnp.sum(e, axis=-1, keepdims=True))).astype(BF)
            o = jnp.dot(w, vs, preferred_element_type=F32).astype(BF)
            for r in range(group):
                parts.append(o[r * QB:(r + 1) * QB, :])
        return jnp.concatenate(parts, axis=1)

    def att_copy(b):
        member, slot = b // bpm, b % bpm
        return pltpu.make_async_remote_copy(
            src_ref=att.at[b], dst_ref=attr.at[tp, slot],
            send_sem=as_sem.at[b], recv_sem=ar_sem.at[tp, slot],
            device_id={"kv": me, "tp": member}, device_id_type=MESH,
        )

    def att_in(t, slot):
        return pltpu.make_async_remote_copy(
            src_ref=att.at[slot], dst_ref=attr.at[t, slot],
            send_sem=as_sem.at[slot], recv_sem=ar_sem.at[t, slot],
            device_id={"kv": me, "tp": t}, device_id_type=MESH,
        )

    for c, pair in enumerate(chunks):
        each(0, me, lambda p, c=c: arrive(c, p).wait_recv())
        for slot, b in enumerate(pair):
            kall[slot, :QB, :] = kv[b * (QB // KB):(b + 1) * (QB // KB)].reshape(QB, 2 * kvw)
            for j in range(nfar):
                owner = jnp.where(j < count, list_s[b, j] // bpg, 0)
                block = recv[c][owner, slot]
                kall[slot, QB + j * KB:QB + (j + 1) * KB, :] = jnp.where(j < count, block, jnp.zeros_like(block))
        for slot, b in enumerate(pair):
            member = b // bpm
            result = attend(b, slot)
            att[b] = result

            @pl.when(tp == member)
            def _(result=result, b=b):
                attr[tp, b % bpm] = result

        for b in pair:
            @pl.when(tp != b // bpm)
            def _(b=b):
                att_copy(b).start()

        if c + 2 < PIECES:
            start_piece(c + 2)
        if c == 1:
            relay_piece(0)
            relay_piece(1)
        if c > 1:
            relay_piece(c)
    for i in range(nch, PIECES):
        relay_piece(i)

    load_wo.wait()
    mate_in.wait_recv()
    for i in range(PIECES):
        for dy in range(1, ny):
            relay(dy, i, sender_of(mate, dy)).wait_recv()
    for slot in range(bpm):
        for i in range(1, ntp):
            att_in(lax.rem(tp + i, ntp), slot).wait_recv()

    width = out_ref.shape[1]
    tile = min(512, width)

    def project_out(n):
        cols = pl.ds(pl.multiple_of(n * tile, tile), tile)
        total = jnp.zeros((bpm * QB, tile), F32)
        for t in range(ntp):
            a = attr[t].reshape(bpm * QB, kd)
            part = jnp.dot(a, wo[t, :, cols], preferred_element_type=F32)
            total = total + part.astype(BF).astype(F32)
        out_ref[:, cols] = total.astype(BF)

    each(0, width // tile, project_out)

    each(0, me, lambda p: table_copy(p).wait_send())
    for c in range(nch):
        each(me + 1, nkv, lambda d, c=c: send_copy(c, d).wait_send())
    mate_copy.wait_send()
    for i in range(PIECES):
        for dy in range(1, ny):
            far_copy(dy, i).wait_send()
            relay(dy, i, sender_of(tp, dy)).wait_send()
    for b in range(blocks):
        @pl.when(tp != b // bpm)
        def _(b=b):
            att_copy(b).wait_send()


def shards(nkv, ntp, tokens, wq, wk, wv, wo, chosen):
    rows, width = tokens.shape
    qw, kvw, kd = wq.shape[1], wk.shape[1], wo.shape[0]
    out_width = wo.shape[1]
    blocks = rows // QB
    nfar = min(chosen.shape[1], nkv - 1)
    bpm = rows // ntp // QB
    keys = -(-(QB + nfar * KB) // 128) * 128
    nch = blocks // 2
    dma = pltpu.SemaphoreType.DMA
    any_spec = pl.BlockSpec(memory_space=pl.ANY)
    return pl.pallas_call(
        functools.partial(kernel, nkv, ntp, nfar),
        out_shape=jax.ShapeDtypeStruct((rows // ntp, out_width), BF),
        in_specs=[any_spec] * 5
        + [pl.BlockSpec(memory_space=pltpu.VMEM), pl.BlockSpec(memory_space=pltpu.SMEM)],
        out_specs=pl.BlockSpec(memory_space=pltpu.VMEM),
        scratch_shapes=[
            pltpu.VMEM((rows, width), BF),
            pltpu.VMEM((width, qw), BF),
            pltpu.VMEM((width, kvw), BF),
            pltpu.VMEM((width, kvw), BF),
            pltpu.VMEM((ntp, kd, out_width), BF),
            pltpu.VMEM((rows, qw), BF),
            pltpu.VMEM((rows // KB, KB, 2 * kvw), BF),
            pltpu.VMEM((blocks, QB, qw), BF),
            pltpu.VMEM((ntp, bpm, QB, qw), BF),
            pltpu.VMEM((2, keys, 2 * kvw), BF),
            pltpu.VMEM((blocks, 128), jnp.int32),
            pltpu.VMEM((nkv, blocks, 128), jnp.int32),
            pltpu.SMEM((nkv, blocks, 128), jnp.int32),
            pltpu.VMEM((nch, nkv, 2, KB, 2 * kvw), BF),
        ]
        + [pltpu.VMEM((nkv, 2, KB, 2 * kvw), BF)] * nch
        + [
            dma((4,)), dma((rows // ROWS,)), dma((nkv,)), dma((nkv,)), dma((nkv,)),
            dma((nch, nkv)), dma((nch, nkv)), dma((blocks,)), dma((ntp, bpm)),
            dma, dma,
            dma((ntp // 2, PIECES)), dma((ntp // 2, PIECES)),
            dma((ntp // 2, PIECES)), dma((ntp // 2, PIECES)),
        ],
        compiler_params=pltpu.CompilerParams(
            collective_id=1, has_side_effects=True, vmem_limit_bytes=58 << 20
        ),
    )(tokens, wq, wk, wv, wo, chosen, chosen)


def solution(mesh):
    return jax.shard_map(
        functools.partial(shards, mesh.shape["kv"], mesh.shape["tp"]),
        mesh=mesh,
        in_specs=(
            P("kv", None),
            P(None, "tp"),
            P(None, "tp"),
            P(None, "tp"),
            P("tp", None),
            P("kv", None),
        ),
        out_specs=P(("kv", "tp"), None),
        check_vma=False,
    )
```

```python
import functools

import jax
import jax.numpy as jnp
from jax import lax
from jax.experimental import pallas as pl
from jax.experimental.pallas import tpu as pltpu
from jax.sharding import PartitionSpec as P

HEAD = 128
QB = 128
KB = 32
PIECES = 4
ROWS = 256
BF = jnp.bfloat16
F32 = jnp.float32
LOG2E = 1.4426950408889634
MESH = pl.DeviceIdType.MESH


def block_pairs(blocks):
    half = blocks // 2
    firsts = list(range(0, half, 2)) + list(range(1, half, 2))
    pairs = [(i, i + half) for i in firsts]
    return pairs[:-1] + [(b,) for b in pairs[-1]]


def kernel(
    nkv, ntp, nfar,
    tok_hbm, wq_hbm, wk_hbm, wv_hbm, wo_hbm, list_v, list_s,
    out_ref,
    tok, wq, wk, wv, wo, q, kv, att, attr, kall, tmine, trecv, tsm, bias, stage, *rest,
):
    chunks = block_pairs(att.shape[0])
    nch = len(chunks)
    recv = rest[:nch]
    (loc_sem, tok_sem, ts_sem, tr_sem, tl_sem, zs_sem, zr_sem,
     as_sem, ar_sem, cs_sem, cr_sem, ys_sem, yr_sem, rs_sem, rr_sem, xs_sem, xr_sem) = rest[nch:]
    me = lax.axis_index("kv")
    tp = lax.axis_index("tp")
    blocks = att.shape[0]
    bpm = attr.shape[1]
    kvw = wk.shape[1]
    kv_heads = kvw // HEAD
    qw = wq.shape[1]
    group = qw // kvw
    bpg = kv.shape[0]
    steps = tok.shape[0] // ROWS
    per_step = ROWS // KB
    kd = wo.shape[1]
    ny = ntp // 2
    mate = tp + 1 - 2 * lax.rem(tp, 2)

    load_wk = pltpu.make_async_copy(wk_hbm, wk, loc_sem.at[0])
    load_wv = pltpu.make_async_copy(wv_hbm, wv, loc_sem.at[1])
    load_wq = pltpu.make_async_copy(wq_hbm, wq, loc_sem.at[2])
    load_wo = pltpu.make_async_copy(wo_hbm, wo.at[tp], loc_sem.at[3])

    def load_tok(s):
        rows = pl.ds(s * ROWS, ROWS)
        return pltpu.make_async_copy(tok_hbm.at[rows, :], tok.at[rows, :], tok_sem.at[s])

    load_wk.start()
    load_tok(0).start()
    load_wv.start()
    for s in range(1, steps):
        load_tok(s).start()

    barrier = pltpu.get_barrier_semaphore()

    def greet(i, c):
        other = lax.rem(me + i, nkv)
        pl.semaphore_signal(barrier, inc=1, device_id={"kv": other, "tp": tp}, device_id_type=MESH)
        return c

    lax.fori_loop(1, nkv, greet, 0)
    for i in range(1, ntp):
        pl.semaphore_signal(
            barrier, inc=1, device_id={"kv": me, "tp": lax.rem(tp + i, ntp)}, device_id_type=MESH
        )

    named = list_v[...]
    lane = lax.broadcasted_iota(jnp.int32, tmine.shape, 1)
    table = jnp.zeros(tmine.shape, jnp.int32)
    for p in range(nkv):
        local = named - p * bpg
        mine = (local >= 0) & (local < bpg)
        column = jnp.sum(jnp.where(mine, local, 0), axis=1, keepdims=True)
        table = jnp.where(lane == p, column, table)
    tmine[...] = table
    pl.semaphore_wait(barrier, nkv + ntp - 2)

    def table_copy(p):
        return pltpu.make_async_remote_copy(
            src_ref=tmine, dst_ref=trecv.at[me], send_sem=ts_sem.at[p], recv_sem=tr_sem.at[me],
            device_id={"kv": p, "tp": tp}, device_id_type=MESH,
        )

    def table_in(d):
        return pltpu.make_async_remote_copy(
            src_ref=tmine, dst_ref=trecv.at[d], send_sem=ts_sem.at[d], recv_sem=tr_sem.at[d],
            device_id={"kv": d, "tp": tp}, device_id_type=MESH,
        )

    def table_local(d):
        return pltpu.make_async_copy(trecv.at[d], tsm.at[d], tl_sem.at[d])

    def each(lower, upper, action):
        def body(i, c):
            action(i)
            return c

        lax.fori_loop(lower, upper, body, 0)

    each(0, me, lambda p: table_copy(p).start())

    piece = kd // PIECES
    mate_copy = pltpu.make_async_remote_copy(
        src_ref=wo_hbm, dst_ref=wo.at[tp], send_sem=cs_sem, recv_sem=cr_sem,
        device_id={"kv": me, "tp": mate}, device_id_type=MESH,
    )
    mate_in = pltpu.make_async_remote_copy(
        src_ref=wo_hbm, dst_ref=wo.at[mate], send_sem=cs_sem, recv_sem=cr_sem,
        device_id={"kv": me, "tp": mate}, device_id_type=MESH,
    )

    parity = lax.rem(me, 2)
    across = me + 1 - 2 * parity

    def piece_rows(i):
        if i == 2:
            i = 2 + parity
        elif i == 3:
            i = 3 - parity
        return pl.ds(pl.multiple_of(i * piece, piece), piece)

    def far_copy(dy, i):
        rows = piece_rows(i)
        return pltpu.make_async_remote_copy(
            src_ref=wo_hbm.at[rows, :], dst_ref=wo.at[tp, rows, :],
            send_sem=ys_sem.at[dy, i], recv_sem=yr_sem.at[dy, i],
            device_id={"kv": me, "tp": lax.rem(tp + 2 * dy, ntp)}, device_id_type=MESH,
        )

    def across_copy(dy, i):
        owner, rows = sender_of(tp, dy), piece_rows(i)
        return pltpu.make_async_remote_copy(
            src_ref=wo.at[owner, rows, :], dst_ref=wo.at[owner, rows, :],
            send_sem=xs_sem.at[dy], recv_sem=xr_sem.at[dy],
            device_id={"kv": across, "tp": tp}, device_id_type=MESH,
        )

    def relay(dy, i, owner):
        rows = piece_rows(i)
        return pltpu.make_async_remote_copy(
            src_ref=wo.at[owner, rows, :], dst_ref=wo.at[owner, rows, :],
            send_sem=rs_sem.at[dy, i], recv_sem=rr_sem.at[dy, i],
            device_id={"kv": me, "tp": mate}, device_id_type=MESH,
        )

    def sender_of(who, dy):
        return lax.rem(who - 2 * dy + ntp, ntp)

    def start_piece(i):
        for dy in range(1, ny):
            far_copy(dy, i).start()

    def relay_piece(i):
        for dy in range(1, ny):
            if i == 3:
                across_copy(dy, 3).wait_recv()
            else:
                far_copy(dy, i).wait_recv()
            if i == 2:
                across_copy(dy, 2).start()
            relay(dy, i, sender_of(tp, dy)).start()

    for i in (2, 0, 1):
        start_piece(i)

    load_wk.wait()
    load_wv.wait()

    def project_kv(s):
        load_tok(s).wait()
        x = tok[pl.ds(s * ROWS, ROWS), :]
        k = jnp.dot(x, wk[...], preferred_element_type=F32).astype(BF)
        v = jnp.dot(x, wv[...], preferred_element_type=F32).astype(BF)
        where = pl.ds(s * per_step, per_step)
        kv[where, :, :kvw] = k.reshape(per_step, KB, kvw)
        kv[where, :, kvw:] = v.reshape(per_step, KB, kvw)

    each(0, steps, project_kv)

    def table_got(d):
        table_in(d).wait_recv()
        table_local(d).start()

    each(me + 1, nkv, table_got)
    each(me + 1, nkv, lambda d: table_local(d).wait())

    def send_copy(c, d):
        return pltpu.make_async_remote_copy(
            src_ref=stage.at[c, d, pl.ds(0, len(chunks[c]))], dst_ref=recv[c].at[me],
            send_sem=zs_sem.at[c, d], recv_sem=zr_sem.at[c, me],
            device_id={"kv": d, "tp": tp}, device_id_type=MESH,
        )

    def arrive(c, p):
        return pltpu.make_async_remote_copy(
            src_ref=stage.at[c, p, pl.ds(0, len(chunks[c]))], dst_ref=recv[c].at[p],
            send_sem=zs_sem.at[c, p], recv_sem=zr_sem.at[c, p],
            device_id={"kv": p, "tp": tp}, device_id_type=MESH,
        )

    load_wq.start()
    later = nkv - 1 - me
    for c, pair in enumerate(chunks):

        def stage_one(i, c=c, pair=pair):
            d = nkv - 1 - i
            for slot, b in enumerate(pair):
                stage[c, d, slot] = kv[tsm[d, b, me]]

        each(0, later, stage_one)
        each(0, later, lambda i, c=c: send_copy(c, nkv - 1 - i).start())

    load_wo.start()
    mate_copy.start()
    load_wq.wait()

    def project_q(s):
        rows = pl.ds(s * ROWS, ROWS)
        q[rows, :] = jnp.dot(tok[rows, :], wq[...], preferred_element_type=F32).astype(BF)

    each(0, steps, project_q)

    keys = kall.shape[1]
    used = QB + nfar * KB
    row = lax.broadcasted_iota(jnp.int32, (QB, keys), 0)
    col = lax.broadcasted_iota(jnp.int32, (QB, keys), 1)
    count = jnp.minimum(nfar, me)
    allowed = (col <= row) | ((col >= QB) & (col < QB + KB * count))
    allowed = jnp.where(allowed, 0.0, -jnp.inf)
    for r in range(group):
        bias[r * QB:(r + 1) * QB, :] = allowed
    if keys > used:
        for slot in range(len(chunks[0])):
            kall[slot, used:, :] = jnp.zeros((keys - used, 2 * kvw), BF)
    scale = HEAD ** (-0.5) * LOG2E

    def attend(b, slot):
        parts = []
        for g in range(kv_heads):
            first = g * group
            qs = jnp.concatenate(
                [q[b * QB:(b + 1) * QB, (first + r) * HEAD:(first + r + 1) * HEAD] for r in range(group)],
                axis=0,
            )
            ks = kall[slot, :, g * HEAD:(g + 1) * HEAD]
            vs = kall[slot, :, kvw + g * HEAD:kvw + (g + 1) * HEAD]
            s = lax.dot_general(qs, ks, (((1,), (1,)), ((), ())), preferred_element_type=F32) * scale
            s = s + bias[...]
            e = jnp.exp2(s - jnp.max(s, axis=-1, keepdims=True))
            w = (e * (1.0 / jnp.sum(e, axis=-1, keepdims=True))).astype(BF)
            o = jnp.dot(w, vs, preferred_element_type=F32).astype(BF)
            for r in range(group):
                parts.append(o[r * QB:(r + 1) * QB, :])
        return jnp.concatenate(parts, axis=1)

    def att_copy(b):
        member, slot = b // bpm, b % bpm
        return pltpu.make_async_remote_copy(
            src_ref=att.at[b], dst_ref=attr.at[tp, slot],
            send_sem=as_sem.at[b], recv_sem=ar_sem.at[tp, slot],
            device_id={"kv": me, "tp": member}, device_id_type=MESH,
        )

    def att_in(t, slot):
        return pltpu.make_async_remote_copy(
            src_ref=att.at[slot], dst_ref=attr.at[t, slot],
            send_sem=as_sem.at[slot], recv_sem=ar_sem.at[t, slot],
            device_id={"kv": me, "tp": t}, device_id_type=MESH,
        )

    def weights_here():
        load_wo.wait()
        mate_in.wait_recv()
        for i in range(PIECES):
            for dy in range(1, ny):
                relay(dy, i, sender_of(mate, dy)).wait_recv()

    width = out_ref.shape[1]
    tile = min(512, width)

    def early(slot):
        return max(c for c, pair in enumerate(chunks) for b in pair if b % bpm == slot) <= nch - 3

    def finish(slot):
        for i in range(1, ntp):
            att_in(lax.rem(tp + i, ntp), slot).wait_recv()

        def project_out(n):
            cols = pl.ds(pl.multiple_of(n * tile, tile), tile)
            total = jnp.zeros((QB, tile), F32)
            for t in range(ntp):
                part = jnp.dot(attr[t, slot], wo[t, :, cols], preferred_element_type=F32)
                total = total + part.astype(BF).astype(F32)
            out_ref[slot * QB:(slot + 1) * QB, cols] = total.astype(BF)

        each(0, width // tile, project_out)

    for c, pair in enumerate(chunks):
        each(0, me, lambda p, c=c: arrive(c, p).wait_recv())
        for slot, b in enumerate(pair):
            kall[slot, :QB, :] = kv[b * (QB // KB):(b + 1) * (QB // KB)].reshape(QB, 2 * kvw)
            for j in range(nfar):
                owner = jnp.where(j < count, list_s[b, j] // bpg, 0)
                block = recv[c][owner, slot]
                kall[slot, QB + j * KB:QB + (j + 1) * KB, :] = jnp.where(j < count, block, jnp.zeros_like(block))
        for slot, b in enumerate(pair):
            member = b // bpm
            result = attend(b, slot)
            att[b] = result

            @pl.when(tp == member)
            def _(result=result, b=b):
                attr[tp, b % bpm] = result

        for b in pair:
            @pl.when(tp != b // bpm)
            def _(b=b):
                att_copy(b).start()

        if c == 0:
            relay_piece(2)
        if c == 1:
            relay_piece(0)
        if c == nch - 3:
            relay_piece(1)
            relay_piece(3)
        if c == nch - 2:
            weights_here()
            for slot in range(bpm):
                if early(slot):
                    finish(slot)

    for slot in range(bpm):
        if not early(slot):
            finish(slot)

    each(0, me, lambda p: table_copy(p).wait_send())
    for c in range(nch):
        each(me + 1, nkv, lambda d, c=c: send_copy(c, d).wait_send())
    mate_copy.wait_send()
    for i in range(PIECES):
        for dy in range(1, ny):
            if i < 3:
                far_copy(dy, i).wait_send()
            if i == 2:
                across_copy(dy, 2).wait_send()
            relay(dy, i, sender_of(tp, dy)).wait_send()
    for b in range(blocks):
        @pl.when(tp != b // bpm)
        def _(b=b):
            att_copy(b).wait_send()


def shards(nkv, ntp, tokens, wq, wk, wv, wo, chosen):
    rows, width = tokens.shape
    qw, kvw, kd = wq.shape[1], wk.shape[1], wo.shape[0]
    out_width = wo.shape[1]
    blocks = rows // QB
    nfar = min(chosen.shape[1], nkv - 1)
    bpm = rows // ntp // QB
    keys = -(-(QB + nfar * KB) // 128) * 128
    chunks = block_pairs(blocks)
    nch = len(chunks)
    group = qw // kvw
    dma = pltpu.SemaphoreType.DMA
    any_spec = pl.BlockSpec(memory_space=pltpu.HBM)
    return pl.pallas_call(
        functools.partial(kernel, nkv, ntp, nfar),
        out_shape=jax.ShapeDtypeStruct((rows // ntp, out_width), BF),
        in_specs=[any_spec] * 5
        + [pl.BlockSpec(memory_space=pltpu.VMEM), pl.BlockSpec(memory_space=pltpu.SMEM)],
        out_specs=pl.BlockSpec(memory_space=pltpu.VMEM),
        scratch_shapes=[
            pltpu.VMEM((rows, width), BF),
            pltpu.VMEM((width, qw), BF),
            pltpu.VMEM((width, kvw), BF),
            pltpu.VMEM((width, kvw), BF),
            pltpu.VMEM((ntp, kd, out_width), BF),
            pltpu.VMEM((rows, qw), BF),
            pltpu.VMEM((rows // KB, KB, 2 * kvw), BF),
            pltpu.VMEM((blocks, QB, qw), BF),
            pltpu.VMEM((ntp, bpm, QB, qw), BF),
            pltpu.VMEM((2, keys, 2 * kvw), BF),
            pltpu.VMEM((blocks, 128), jnp.int32),
            pltpu.VMEM((nkv, blocks, 128), jnp.int32),
            pltpu.SMEM((nkv, blocks, 128), jnp.int32),
            pltpu.VMEM((group * QB, keys), F32),
            pltpu.VMEM((nch, nkv, 2, KB, 2 * kvw), BF),
        ]
        + [pltpu.VMEM((nkv, len(pair), KB, 2 * kvw), BF) for pair in chunks]
        + [
            dma((4,)), dma((rows // ROWS,)), dma((nkv,)), dma((nkv,)), dma((nkv,)),
            dma((nch, nkv)), dma((nch, nkv)), dma((blocks,)), dma((ntp, bpm)),
            dma, dma,
            dma((ntp // 2, PIECES)), dma((ntp // 2, PIECES)),
            dma((ntp // 2, PIECES)), dma((ntp // 2, PIECES)),
            dma((ntp // 2,)), dma((ntp // 2,)),
        ],
        compiler_params=pltpu.CompilerParams(
            collective_id=1, has_side_effects=True, vmem_limit_bytes=52 << 20
        ),
    )(tokens, wq, wk, wv, wo, chosen, chosen)


def solution(mesh):
    return jax.shard_map(
        functools.partial(shards, mesh.shape["kv"], mesh.shape["tp"]),
        mesh=mesh,
        in_specs=(
            P("kv", None),
            P(None, "tp"),
            P(None, "tp"),
            P(None, "tp"),
            P("tp", None),
            P("kv", None),
        ),
        out_specs=P(("kv", "tp"), None),
        check_vma=False,
    )
```
